32 devices in a mesh: fs: 8 (over z, y), tp: 4 (over x, core).
Axes of the slice: x: 2, y: 2, z: 4, core: 2. Of those that a mesh axis runs over, the one named last changes fastest.
Arguments:
- inputs: bfloat16 [16384, 2048], P('fs'), may hold values from -6 to 6
- cotangents: bfloat16 [3, 16384, 1024], P(None, 'fs', 'tp'), as said below
- factor: bfloat16 [2048, 256], P('fs'), as said below
- weights: float32 [3, 2048, 1024], P(None, 'fs', 'tp'), may hold values from -0.125 to 0.125
- first_moment: float32 [3, 256, 1024], P(None, 'fs', 'tp'), may hold values from -0.6 to 0.6
- second_moment: float32 [3, 256, 1024], P(None, 'fs', 'tp'), may hold values from 0.001 to 0.01
Outputs:
- update: float32 [3, 2048, 1024], P(None, 'fs', 'tp')
- new_weights: float32 [3, 2048, 1024], P(None, 'fs', 'tp')
- copies: bfloat16 [3, 2048, 1024], P(None, None, 'tp')
- new_first: float32 [3, 256, 1024], P(None, 'fs', 'tp')
- new_second: float32 [3, 256, 1024], P(None, 'fs', 'tp')
The draws below stay inside these ranges and needn't reach their ends.
Inputs may be any that keep to these rules, and one draw needn't show every extreme that they name: A real-valued factor of full rank. real-valued cotangents.
All inputs are finite; a program needn't handle non-finite values.
Results may differ from the reference program's by a relative error of at most 0.0085.
Values may be sent and summed in bfloat16 or wider, within the bound.
A program may use at most 64 MiB of HBM per device.

```python
import math
import jax
import jax.numpy as jnp
from jax import lax

D = 2048
MW = 1024
RANK = 256
TOKENS = 16384


def draw_cotangents(key, part):
    first_key = jax.random.fold_in(jax.random.fold_in(key, 11), 0)
    columns = jnp.arange(MW, dtype=jnp.float32) / max(MW - 1, 1)
    base = jnp.clip(jax.random.normal(first_key, (3, TOKENS, MW), jnp.float32), -6.0, 6.0)
    spread = jnp.power(4.0, columns)
    values = base * spread / TOKENS ** 0.5
    return values.astype(jnp.bfloat16)


def draw_factor(key, part):
    first_key = jax.random.fold_in(key, 23)
    columns = jnp.arange(RANK, dtype=jnp.float32) / max(RANK - 1, 1)
    base = jnp.clip(jax.random.normal(first_key, (D, RANK), jnp.float32), -6.0, 6.0)
    spread = jnp.power(3.0, columns)
    values = base * spread / D ** 0.5
    return values.astype(jnp.bfloat16)


def steps_of(key, extent, cuts, low, high):
    gain, own = 1.0, jax.random.fold_in(key, 6)
    for position, shards_of in cuts:
        heights = jnp.exp(jax.random.uniform(jax.random.fold_in(own, position), (shards_of,), jnp.float32, low / len(cuts), high / len(cuts)))
        gain = gain * jnp.repeat(heights, extent[position] // shards_of).reshape([-1 if axis == position else 1 for axis in range(len(extent))])
    return gain


def bell_draw(own_key, extent, deviation, most, pieces=(), kind=jnp.bfloat16):
    drawn = deviation * jax.random.normal(own_key, extent, jnp.float32)
    if pieces:
        drawn = drawn * steps_of(own_key, extent, pieces, -0.22, 0.18)
    return jnp.clip(drawn, -most, most).astype(kind)


def setup_inputs(seed: int = 0) -> dict:
    key_list = jax.random.split(jax.random.key(seed), 7)
    inputs = bell_draw(key_list[0], (TOKENS, D), 1.0, 6.0, ((0, 8),))
    cotangents = draw_cotangents(jax.random.fold_in(key_list[6], 71), 0)
    factor = draw_factor(jax.random.fold_in(key_list[6], 71), 0)
    weights = bell_draw(key_list[3], (3, D, MW), D ** -0.5, 0.125, ((1, 8), (2, 4)), jnp.float32)
    first_moment = bell_draw(key_list[4], (3, RANK, MW), 0.1, 0.6, ((1, 8), (2, 4)), jnp.float32)
    second_moment = jnp.clip(jnp.exp(math.log(0.01) - 2.30258502 * jax.random.uniform(key_list[5], (3, RANK, MW), jnp.float32) ** steps_of(key_list[5], (3, RANK, MW), ((1, 8), (2, 4)), -0.2, 0.2)), 0.001, 0.01)
    return {"inputs": inputs, "cotangents": cotangents, "factor": factor, "weights": weights, "first_moment": first_moment, "second_moment": second_moment}


def reference(inputs, cotangents, factor, weights, first_moment, second_moment):
    factor_wide = factor.astype(jnp.float32)
    projected_list = []
    for which in range(3):
        gradient = jnp.dot(inputs.T, cotangents[which], preferred_element_type=jnp.float32)
        projected_list.append(jnp.dot(factor_wide.T, gradient, precision=lax.Precision.HIGHEST))
    projected = jnp.stack(projected_list)
    square_sum = jnp.sum(projected * projected)
    root_mean = jnp.sqrt(square_sum / (3 * RANK * MW) + 1e-06)
    clip_factor = jnp.minimum(1.0, 0.25 / root_mean)
    clipped = clip_factor * projected
    new_first = 0.9 * first_moment + 0.1 * clipped
    new_second = 0.95 * second_moment + 0.05 * clipped * clipped
    normed = new_first / (jnp.sqrt(new_second) + 1e-08)
    update = jnp.einsum('dr,mrc->mdc', factor_wide, normed, precision=lax.Precision.HIGHEST)
    new_weights = weights - 0.02 * update
    copies = new_weights.astype(jnp.bfloat16)
    return (update, new_weights, copies, new_first, new_second)
```

```python
import functools

import jax
import jax.numpy as jnp
from jax import lax
from jax.experimental import pallas as pl
from jax.experimental.pallas import tpu as pltpu
from jax.sharding import PartitionSpec as P

MESH = pl.DeviceIdType.MESH


def flip(index, bits, count):
    result, weight = 0, 1
    while weight < count:
        bit = (bits // weight) % 2
        result = result + lax.rem(lax.div(index, weight) + bit, 2) * weight
        weight *= 2
    return result


def exchange_kernel(
    nfs, ntp, scale_count,
    x_hbm, c_hbm, f_ref, first_in, second_in,
    first_ref, second_ref, f_out, normed_out,
    xbuf, cbuf, pacc, fbuf, pbuf, rbuf, nbuf, sq_own, sq_tp, sq_mid, sq_fs,
    x_sem, c_sem, fo_sem,
    f_send, f_recv, d_send, d_recv, p_send, p_recv,
    t_send, t_recv, s_send, s_recv, n_send, n_recv,
):
    me, col = lax.axis_index("fs"), lax.axis_index("tp")
    core = lax.rem(col, 2)
    mate = flip(col, 1, ntp)
    chunks, chunk = xbuf.shape[0], xbuf.shape[1]
    rows = first_in.shape[1]
    peers = [flip(me, o, nfs) for o in range(1, nfs)]
    sides = [flip(col, o, ntp) for o in range(1, ntp)]

    def remote(src, dst, send, recv, fs, tp):
        return pltpu.make_async_remote_copy(
            src_ref=src, dst_ref=dst, send_sem=send, recv_sem=recv,
            device_id=(fs, tp), device_id_type=MESH,
        )

    x_copies = [
        pltpu.make_async_copy(x_hbm.at[i], xbuf.at[i], x_sem.at[i]) for i in range(chunks)
    ]
    c_copies = [pltpu.make_async_copy(c_hbm.at[m], cbuf.at[m], c_sem.at[m]) for m in range(3)]
    for copy in x_copies + c_copies:
        copy.start()

    barrier = pltpu.get_barrier_semaphore()
    for peer in peers:
        pl.semaphore_signal(barrier, inc=1, device_id=(peer, col), device_id_type=MESH)
    for side in sides:
        pl.semaphore_signal(barrier, inc=1, device_id=(me, side), device_id_type=MESH)
    pl.semaphore_wait(barrier, nfs - 1 + ntp - 1)

    sends = []
    for o, peer in enumerate(peers):
        copy = remote(f_ref.at[core], fbuf.at[me, core], f_send.at[o], f_recv.at[me], peer, col)
        copy.start()
        sends.append(copy)
    fbuf[me] = f_ref[...]
    for o, peer in enumerate(peers):
        remote(
            f_ref.at[core], fbuf.at[peer, core], f_send.at[o], f_recv.at[peer], peer, col
        ).wait_recv()
        copy = remote(
            fbuf.at[peer, core], fbuf.at[peer, core], d_send.at[o], d_recv.at[peer], me, mate
        )
        copy.start()
        sends.append(copy)
    for copy in x_copies + c_copies:
        copy.wait()
    for o, peer in enumerate(peers):
        remote(
            f_ref.at[core], fbuf.at[peer, 1 - core], d_send.at[o], d_recv.at[peer], me, mate
        ).wait_recv()
    f_copy = pltpu.make_async_copy(fbuf, f_out, fo_sem)
    f_copy.start()

    pacc[...] = jnp.zeros_like(pacc)
    whole = fbuf.shape[0] * fbuf.shape[1] * fbuf.shape[2]

    @pl.loop(0, chunks)
    def _(i):
        factor = fbuf[...].reshape(whole, fbuf.shape[3])
        low = jnp.dot(xbuf[i], factor, preferred_element_type=jnp.float32).astype(jnp.bfloat16)
        for m in range(3):
            tokens = pl.ds(pl.multiple_of(i * chunk, chunk), chunk)
            pacc[m] += lax.dot_general(
                low, cbuf[m, tokens, :], (((0,), (0,)), ((), ())),
                preferred_element_type=jnp.float32,
            )

    for m in range(3):
        for j in range(nfs):
            pbuf[j, m] = pacc[m, j * rows:(j + 1) * rows, :].astype(jnp.bfloat16)
    for o, peer in enumerate(peers):
        copy = remote(pbuf.at[peer], rbuf.at[me], p_send.at[o], p_recv.at[me], peer, col)
        copy.start()
        sends.append(copy)
    projected = pacc[:, pl.ds(pl.multiple_of(me * rows, rows), rows), :]
    for o, peer in enumerate(peers):
        remote(
            pbuf.at[peer], rbuf.at[peer], p_send.at[o], p_recv.at[peer], peer, col
        ).wait_recv()
        projected = projected + rbuf[peer].astype(jnp.float32)

    def spread(value):
        total = jnp.sum(jnp.sum(value, axis=0), axis=0, keepdims=True)
        return jnp.broadcast_to(jnp.sum(total, axis=1, keepdims=True), sq_own.shape)

    own = spread(projected * projected)
    sq_own[...] = own
    sq_tp[col] = own
    for o, side in enumerate(sides):
        copy = remote(sq_own, sq_tp.at[col], t_send.at[o], t_recv.at[col], me, side)
        copy.start()
        sends.append(copy)
    for o, side in enumerate(sides):
        remote(sq_own, sq_tp.at[side], t_send.at[o], t_recv.at[side], me, side).wait_recv()
    mid = jnp.sum(sq_tp[...], axis=0)
    sq_mid[...] = mid
    sq_fs[me] = mid
    for o, peer in enumerate(peers):
        copy = remote(sq_mid, sq_fs.at[me], s_send.at[o], s_recv.at[me], peer, col)
        copy.start()
        sends.append(copy)
    for o, peer in enumerate(peers):
        remote(sq_mid, sq_fs.at[peer], s_send.at[o], s_recv.at[peer], peer, col).wait_recv()
    square_sum = jnp.sum(sq_fs[...], axis=0)[:, :1]

    root_mean = jnp.sqrt(square_sum / scale_count + 1e-06)
    clip_factor = jnp.minimum(1.0, 0.25 / root_mean)
    clipped = clip_factor * projected
    new_first = 0.9 * first_in[...] + 0.1 * clipped
    new_second = 0.95 * second_in[...] + 0.05 * clipped * clipped
    normed = new_first / (jnp.sqrt(new_second) + 1e-08)
    nbuf[me] = normed.astype(jnp.bfloat16)
    for o, peer in enumerate(peers):
        copy = remote(nbuf.at[me], nbuf.at[me], n_send.at[o], n_recv.at[me], peer, col)
        copy.start()
        sends.append(copy)
    first_ref[...] = new_first
    second_ref[...] = new_second
    for o, peer in enumerate(peers):
        remote(
            nbuf.at[peer], nbuf.at[peer], n_send.at[o], n_recv.at[peer], peer, col
        ).wait_recv()
    for m in range(3):
        normed_out[m] = jnp.concatenate(
            [nbuf[j, m].astype(jnp.float32) for j in range(nfs)], axis=0
        ).astype(jnp.bfloat16)
    f_copy.wait()
    for copy in sends:
        copy.wait_send()


def finish_kernel(f_ref, f_all, normed, weights, gathered, update, new_weights, copies):
    step = jnp.dot(f_ref[...], normed[0], preferred_element_type=jnp.float32)
    update[0] = step
    new_weights[0] = weights[0] - 0.02 * step
    held = gathered.shape[2]
    for j in range(gathered.shape[0]):
        step = jnp.dot(f_all[j], normed[0], preferred_element_type=jnp.float32)
        copies[0, j * held:(j + 1) * held] = (
            gathered[j, 0].astype(jnp.float32) - 0.02 * step
        ).astype(jnp.bfloat16)


def on_device(nfs, ntp, inputs, cotangents, factor, weights, first_moment, second_moment):
    tokens, width = inputs.shape
    held, rank = factor.shape
    rows, cols = first_moment.shape[1:]
    chunk = min(512, tokens)
    chunks = tokens // chunk
    gathered = lax.all_gather(weights.astype(jnp.bfloat16), "fs", axis=0)

    dma = pltpu.SemaphoreType.DMA
    vmem = pl.BlockSpec(memory_space=pltpu.VMEM)
    hbm = pl.BlockSpec(memory_space=pl.ANY)
    new_first, new_second, f_all, normed = pl.pallas_call(
        functools.partial(exchange_kernel, nfs, ntp, 3 * rank * cols * ntp),
        out_shape=(
            jax.ShapeDtypeStruct(first_moment.shape, jnp.float32),
            jax.ShapeDtypeStruct(second_moment.shape, jnp.float32),
            jax.ShapeDtypeStruct((nfs, 2, held // 2, rank), jnp.bfloat16),
            jax.ShapeDtypeStruct((3, rank, cols), jnp.bfloat16),
        ),
        in_specs=[hbm, hbm, vmem, vmem, vmem],
        out_specs=(vmem, vmem, hbm, vmem),
        scratch_shapes=[
            pltpu.VMEM((chunks, chunk, width), jnp.bfloat16),
            pltpu.VMEM(cotangents.shape, jnp.bfloat16),
            pltpu.VMEM((3, rank, cols), jnp.float32),
            pltpu.VMEM((nfs, 2, held // 2, rank), jnp.bfloat16),
            pltpu.VMEM((nfs, 3, rows, cols), jnp.bfloat16),
            pltpu.VMEM((nfs, 3, rows, cols), jnp.bfloat16),
            pltpu.VMEM((nfs, 3, rows, cols), jnp.bfloat16),
            pltpu.VMEM((1, 128), jnp.float32),
            pltpu.VMEM((ntp, 1, 128), jnp.float32),
            pltpu.VMEM((1, 128), jnp.float32),
            pltpu.VMEM((nfs, 1, 128), jnp.float32),
            dma((chunks,)), dma((3,)), dma,
            dma((nfs,)), dma((nfs,)), dma((nfs,)), dma((nfs,)), dma((nfs,)), dma((nfs,)),
            dma((ntp,)), dma((ntp,)), dma((nfs,)), dma((nfs,)), dma((nfs,)), dma((nfs,)),
        ],
        compiler_params=pltpu.CompilerParams(
            collective_id=0, has_side_effects=True, vmem_limit_bytes=63 * 2**20
        ),
        cost_estimate=pl.CostEstimate(
            flops=50_000_000_000, bytes_accessed=100_000_000, transcendentals=0
        ),
        name="exchange",
    )(
        inputs.reshape(chunks, chunk, width), cotangents,
        factor.reshape(2, held // 2, rank), first_moment, second_moment,
    )
    f_all = f_all.reshape(nfs, held, rank)
    update, new_weights, copies = pl.pallas_call(
        finish_kernel,
        grid=(3,),
        out_shape=(
            jax.ShapeDtypeStruct(weights.shape, jnp.float32),
            jax.ShapeDtypeStruct(weights.shape, jnp.float32),
            jax.ShapeDtypeStruct((3, nfs * held, cols), jnp.bfloat16),
        ),
        in_specs=[
            pl.BlockSpec((held, rank), lambda m: (0, 0)),
            pl.BlockSpec((nfs, held, rank), lambda m: (0, 0, 0)),
            pl.BlockSpec((1, rank, cols), lambda m: (m, 0, 0)),
            pl.BlockSpec((1, held, cols), lambda m: (m, 0, 0)),
            pl.BlockSpec((nfs, 1, held, cols), lambda m: (0, m, 0, 0)),
        ],
        out_specs=(
            pl.BlockSpec((1, held, cols), lambda m: (m, 0, 0)),
            pl.BlockSpec((1, held, cols), lambda m: (m, 0, 0)),
            pl.BlockSpec((1, nfs * held, cols), lambda m: (m, 0, 0)),
        ),
        name="finish",
    )(factor, f_all, normed, weights, gathered)
    return (update, new_weights, copies, new_first, new_second)


def solution(mesh):
    placed = (
        P("fs", None),
        P(None, "fs", "tp"),
        P("fs", None),
        P(None, "fs", "tp"),
        P(None, "fs", "tp"),
        P(None, "fs", "tp"),
    )
    return jax.shard_map(
        functools.partial(on_device, mesh.shape["fs"], mesh.shape["tp"]),
        mesh=mesh,
        in_specs=placed,
        out_specs=(
            P(None, "fs", "tp"),
            P(None, "fs", "tp"),
            P(None, None, "tp"),
            P(None, "fs", "tp"),
            P(None, "fs", "tp"),
        ),
        check_vma=False,
    )
```

```python
import functools

import jax
import jax.numpy as jnp
from jax import lax
from jax.experimental import pallas as pl
from jax.experimental.pallas import tpu as pltpu
from jax.sharding import PartitionSpec as P

MESH = pl.DeviceIdType.MESH


def flip(index, bits, count):
    result, weight = 0, 1
    while weight < count:
        bit = (bits // weight) % 2
        result = result + lax.rem(lax.div(index, weight) + bit, 2) * weight
        weight *= 2
    return result


def ring_index(place, count):
    place = lax.rem(place + count, count)
    odd = lax.div(place, count // 2)
    return (1 - odd) * 2 * place + odd * (2 * (count - 1 - place) + 1)


def exchange_kernel(
    nfs, ntp, scale_count,
    x_hbm, c_hbm, f_hbm, w_hbm, first_hbm, second_hbm,
    first_ref, second_ref, f_out, normed_out, w_out,
    xbuf, cbuf, wide, first_in, second_in,
    pacc, fbuf, wbuf, pbuf, rbuf, nbuf, sq_own, sq_tp, sq_mid, sq_fs,
    x_sem, c_sem, in_sem, fo_sem, wo_sem,
    f_send, f_recv, d_send, d_recv, w_send, w_recv, p_send, p_recv,
    t_send, t_recv, s_send, s_recv, n_send, n_recv,
):
    me, col = lax.axis_index("fs"), lax.axis_index("tp")
    core = lax.rem(col, 2)
    mate = flip(col, 1, ntp)
    chunks, chunk = xbuf.shape[0], xbuf.shape[1]
    rows = first_in.shape[1]
    half = wbuf.shape[3]
    peers = [flip(me, o, nfs) for o in range(1, nfs)]
    sides = [flip(col, o, ntp) for o in range(1, ntp)]
    odd = lax.rem(me, 2)
    place = (1 - odd) * lax.div(me, 2) + odd * (nfs - 1 - lax.div(me, 2))
    onward = [ring_index(place + 1, nfs), ring_index(place - 1, nfs)]
    hops = [nfs // 2, (nfs - 1) // 2]
    sends = []

    def origin(way, step):
        return ring_index(place - step if way == 0 else place + step, nfs)

    def remote(src, dst, send, recv, fs, tp):
        return pltpu.make_async_remote_copy(
            src_ref=src, dst_ref=dst, send_sem=send, recv_sem=recv,
            device_id=(fs, tp), device_id_type=MESH,
        )

    def begin(copy):
        copy.start()
        sends.append(copy)

    f_copy = pltpu.make_async_copy(f_hbm, fbuf.at[me], in_sem.at[0])
    w_copy = pltpu.make_async_copy(w_hbm, wide, in_sem.at[1])
    moments = [
        pltpu.make_async_copy(first_hbm, first_in, in_sem.at[2]),
        pltpu.make_async_copy(second_hbm, second_in, in_sem.at[3]),
    ]
    x_copies = [
        pltpu.make_async_copy(x_hbm.at[i], xbuf.at[i], x_sem.at[i]) for i in range(chunks)
    ]
    c_copies = [pltpu.make_async_copy(c_hbm.at[m], cbuf.at[m], c_sem.at[m]) for m in range(3)]
    for copy in [f_copy, w_copy] + x_copies + c_copies + moments:
        copy.start()

    barrier = pltpu.get_barrier_semaphore()
    for peer in peers:
        pl.semaphore_signal(barrier, inc=1, device_id=(peer, col), device_id_type=MESH)
    for side in sides:
        pl.semaphore_signal(barrier, inc=1, device_id=(me, side), device_id_type=MESH)
    f_copy.wait()
    w_copy.wait()
    for way in range(2):
        for m in range(3):
            wbuf[me, way, m] = wide[m, way * half:(way + 1) * half, :].astype(jnp.bfloat16)
    pl.semaphore_wait(barrier, nfs - 1 + ntp - 1)

    def pass_weights(way, step, m):
        held = wbuf.at[origin(way, step), way, m]
        return remote(
            held, held, w_send.at[way, m, step], w_recv.at[way, m, origin(way, step)],
            onward[way], col,
        )

    stores = []

    def store_weights(way, step):
        where = origin(way, step)
        copy = pltpu.make_async_copy(
            wbuf.at[where, way], w_out.at[where, way], wo_sem.at[way, step]
        )
        copy.start()
        stores.append(copy)

    ticks = [(step, m) for step in range(1, nfs) for m in range(3)]
    total_ticks = len(ticks)

    def advance(part):
        while ticks and (total_ticks - len(ticks)) * 21 < part * total_ticks:
            step, m = ticks.pop(0)
            for way in range(2):
                pass_weights(way, step, m).wait_recv()
                if step < nfs - 1:
                    begin(pass_weights(way, step, m))
                if m == 2:
                    store_weights(way, step)

    def pass_factor(way, step):
        held = fbuf.at[origin(way, step), core]
        return remote(
            held, held, f_send.at[way, step], f_recv.at[origin(way, step)], onward[way], col
        )

    def share_factor(way, step, which):
        held = fbuf.at[origin(way, step), which]
        return remote(
            held, held, d_send.at[way, step], d_recv.at[origin(way, step)], me, mate
        )

    for way in range(2):
        begin(pass_factor(way, 0))
    for step in range(1, hops[0] + 1):
        for way in range(2):
            if step <= hops[way]:
                pass_factor(way, step).wait_recv()
                if step < hops[way]:
                    begin(pass_factor(way, step))
                begin(share_factor(way, step, core))
        if step <= 3:
            for way in range(2):
                begin(pass_weights(way, 0, step - 1))
                if step == 3:
                    store_weights(way, 0)
    for copy in x_copies + c_copies:
        copy.wait()
    for way in range(2):
        for step in range(1, hops[way] + 1):
            share_factor(way, step, 1 - core).wait_recv()
    fo_copy = pltpu.make_async_copy(fbuf, f_out, fo_sem)
    fo_copy.start()

    pacc[...] = jnp.zeros_like(pacc)
    whole = fbuf.shape[0] * fbuf.shape[1] * fbuf.shape[2]
    for i in range(chunks):
        factor = fbuf[...].reshape(whole, fbuf.shape[3])
        low = jnp.dot(xbuf[i], factor, preferred_element_type=jnp.float32).astype(jnp.bfloat16)
        for m in range(3):
            pacc[m] += lax.dot_general(
                low, cbuf[m, i * chunk:(i + 1) * chunk, :], (((0,), (0,)), ((), ())),
                preferred_element_type=jnp.float32,
            )
        if i < chunks - 1:
            advance(i + 1)

    for m in range(3):
        for j in range(nfs):
            pbuf[j, m] = pacc[m, j * rows:(j + 1) * rows, :].astype(jnp.bfloat16)
    for o, peer in enumerate(peers):
        begin(remote(pbuf.at[peer], rbuf.at[me], p_send.at[o], p_recv.at[me], peer, col))
    projected = pacc[:, pl.ds(pl.multiple_of(me * rows, rows), rows), :]
    for o, peer in enumerate(peers):
        advance(4 + (o * 6) // len(peers))
        remote(
            pbuf.at[peer], rbuf.at[peer], p_send.at[o], p_recv.at[peer], peer, col
        ).wait_recv()
        projected = projected + rbuf[peer].astype(jnp.float32)

    def spread(value):
        total = jnp.sum(jnp.sum(value, axis=0), axis=0, keepdims=True)
        return jnp.broadcast_to(jnp.sum(total, axis=1, keepdims=True), sq_own.shape)

    own = spread(projected * projected)
    sq_own[...] = own
    sq_tp[col] = own
    for o, side in enumerate(sides):
        begin(remote(sq_own, sq_tp.at[col], t_send.at[o], t_recv.at[col], me, side))
    advance(11)
    for o, side in enumerate(sides):
        remote(sq_own, sq_tp.at[side], t_send.at[o], t_recv.at[side], me, side).wait_recv()
    mid = jnp.sum(sq_tp[...], axis=0)
    sq_mid[...] = mid
    sq_fs[me] = mid
    for o, peer in enumerate(peers):
        begin(remote(sq_mid, sq_fs.at[me], s_send.at[o], s_recv.at[me], peer, col))
    for copy in moments:
        copy.wait()
    advance(13)
    for o, peer in enumerate(peers):
        remote(sq_mid, sq_fs.at[peer], s_send.at[o], s_recv.at[peer], peer, col).wait_recv()
    square_sum = jnp.sum(sq_fs[...], axis=0)[:, :1]

    root_mean = jnp.sqrt(square_sum / scale_count + 1e-06)
    clip_factor = jnp.minimum(1.0, 0.25 / root_mean)
    clipped = clip_factor * projected
    new_first = 0.9 * first_in[...] + 0.1 * clipped
    new_second = 0.95 * second_in[...] + 0.05 * clipped * clipped
    normed = new_first / (jnp.sqrt(new_second) + 1e-08)
    nbuf[me] = normed.astype(jnp.bfloat16)

    def pass_normed(way, step):
        held = nbuf.at[origin(way, step)]
        return remote(
            held, held, n_send.at[way, step], n_recv.at[origin(way, step)], onward[way], col
        )

    for way in range(2):
        begin(pass_normed(way, 0))
    first_ref[...] = new_first
    second_ref[...] = new_second
    for step in range(1, hops[0] + 1):
        advance(13 + (step * 7) // hops[0])
        for way in range(2):
            if step <= hops[way]:
                pass_normed(way, step).wait_recv()
                if step < hops[way]:
                    begin(pass_normed(way, step))
    for m in range(3):
        normed_out[m] = jnp.concatenate(
            [nbuf[j, m].astype(jnp.float32) for j in range(nfs)], axis=0
        ).astype(jnp.bfloat16)
    advance(21)
    fo_copy.wait()
    for copy in stores:
        copy.wait()
    for copy in sends:
        copy.wait_send()


def finish_kernel(f_ref, f_all, normed, weights, gathered, update, new_weights, copies):
    step = jnp.dot(f_ref[...], normed[0], preferred_element_type=jnp.float32)
    update[0] = step
    new_weights[0] = weights[0] - 0.02 * step
    pieces, _, _, half, cols = gathered.shape
    for j in range(pieces):
        step = jnp.dot(f_all[j], normed[0], preferred_element_type=jnp.float32)
        copies[0, j * 2 * half:(j + 1) * 2 * half] = (
            gathered[j, :, 0].astype(jnp.float32).reshape(2 * half, cols) - 0.02 * step
        ).astype(jnp.bfloat16)


def on_device(nfs, ntp, inputs, cotangents, factor, weights, first_moment, second_moment):
    tokens, width = inputs.shape
    held, rank = factor.shape
    rows, cols = first_moment.shape[1:]
    chunk = min(512, tokens)
    chunks = tokens // chunk

    dma = pltpu.SemaphoreType.DMA
    vmem = pl.BlockSpec(memory_space=pltpu.VMEM)
    hbm = pl.BlockSpec(memory_space=pl.ANY)
    new_first, new_second, f_all, normed, gathered = pl.pallas_call(
        functools.partial(exchange_kernel, nfs, ntp, 3 * rank * cols * ntp),
        out_shape=(
            jax.ShapeDtypeStruct(first_moment.shape, jnp.float32),
            jax.ShapeDtypeStruct(second_moment.shape, jnp.float32),
            jax.ShapeDtypeStruct((nfs, 2, held // 2, rank), jnp.bfloat16),
            jax.ShapeDtypeStruct((3, rank, cols), jnp.bfloat16),
            jax.ShapeDtypeStruct((nfs, 2, 3, held // 2, cols), jnp.bfloat16),
        ),
        in_specs=[hbm] * 6,
        out_specs=(vmem, vmem, hbm, vmem, hbm),
        scratch_shapes=[
            pltpu.VMEM((chunks, chunk, width), jnp.bfloat16),
            pltpu.VMEM(cotangents.shape, jnp.bfloat16),
            pltpu.VMEM(weights.shape, jnp.float32),
            pltpu.VMEM(first_moment.shape, jnp.float32),
            pltpu.VMEM(second_moment.shape, jnp.float32),
            pltpu.VMEM((3, rank, cols), jnp.float32),
            pltpu.VMEM((nfs, 2, held // 2, rank), jnp.bfloat16),
            pltpu.VMEM((nfs, 2, 3, held // 2, cols), jnp.bfloat16),
            pltpu.VMEM((nfs, 3, rows, cols), jnp.bfloat16),
            pltpu.VMEM((nfs, 3, rows, cols), jnp.bfloat16),
            pltpu.VMEM((nfs, 3, rows, cols), jnp.bfloat16),
            pltpu.VMEM((1, 128), jnp.float32),
            pltpu.VMEM((ntp, 1, 128), jnp.float32),
            pltpu.VMEM((1, 128), jnp.float32),
            pltpu.VMEM((nfs, 1, 128), jnp.float32),
            dma((chunks,)), dma((3,)), dma((4,)), dma, dma((2, nfs)),
            dma((2, nfs)), dma((nfs,)), dma((2, nfs)), dma((nfs,)),
            dma((2, 3, nfs)), dma((2, 3, nfs)), dma((nfs,)), dma((nfs,)),
            dma((ntp,)), dma((ntp,)), dma((nfs,)), dma((nfs,)), dma((2, nfs)), dma((nfs,)),
        ],
        compiler_params=pltpu.CompilerParams(
            collective_id=0, has_side_effects=True, vmem_limit_bytes=63 * 2**20
        ),
        cost_estimate=pl.CostEstimate(
            flops=50_000_000_000, bytes_accessed=100_000_000, transcendentals=0
        ),
        name="exchange",
    )(
        inputs.reshape(chunks, chunk, width), cotangents,
        factor.reshape(2, held // 2, rank), weights, first_moment, second_moment,
    )
    f_all = f_all.reshape(nfs, held, rank)
    update, new_weights, copies = pl.pallas_call(
        finish_kernel,
        grid=(3,),
        out_shape=(
            jax.ShapeDtypeStruct(weights.shape, jnp.float32),
            jax.ShapeDtypeStruct(weights.shape, jnp.float32),
            jax.ShapeDtypeStruct((3, nfs * held, cols), jnp.bfloat16),
        ),
        in_specs=[
            pl.BlockSpec((held, rank), lambda m: (0, 0)),
            pl.BlockSpec((nfs, held, rank), lambda m: (0, 0, 0)),
            pl.BlockSpec((1, rank, cols), lambda m: (m, 0, 0)),
            pl.BlockSpec((1, held, cols), lambda m: (m, 0, 0)),
            pl.BlockSpec((nfs, 2, 1, held // 2, cols), lambda m: (0, 0, m, 0, 0)),
        ],
        out_specs=(
            pl.BlockSpec((1, held, cols), lambda m: (m, 0, 0)),
            pl.BlockSpec((1, held, cols), lambda m: (m, 0, 0)),
            pl.BlockSpec((1, nfs * held, cols), lambda m: (m, 0, 0)),
        ),
        name="finish",
    )(factor, f_all, normed, weights, gathered)
    return (update, new_weights, copies, new_first, new_second)


def solution(mesh):
    placed = (
        P("fs", None),
        P(None, "fs", "tp"),
        P("fs", None),
        P(None, "fs", "tp"),
        P(None, "fs", "tp"),
        P(None, "fs", "tp"),
    )
    return jax.shard_map(
        functools.partial(on_device, mesh.shape["fs"], mesh.shape["tp"]),
        mesh=mesh,
        in_specs=placed,
        out_specs=(
            P(None, "fs", "tp"),
            P(None, "fs", "tp"),
            P(None, None, "tp"),
            P(None, "fs", "tp"),
            P(None, "fs", "tp"),
        ),
        check_vma=False,
    )
```

```python
import functools

import jax
import jax.numpy as jnp
from jax import lax
from jax.experimental import pallas as pl
from jax.experimental.pallas import tpu as pltpu
from jax.sharding import PartitionSpec as P

MESH = pl.DeviceIdType.MESH


def flip(index, bits, count):
    result, weight = 0, 1
    while weight < count:
        bit = (bits // weight) % 2
        result = result + lax.rem(lax.div(index, weight) + bit, 2) * weight
        weight *= 2
    return result


def ring_index(place, count):
    place = lax.rem(place + count, count)
    odd = lax.div(place, count // 2)
    return (1 - odd) * 2 * place + odd * (2 * (count - 1 - place) + 1)


def exchange_kernel(
    nfs, ntp, scale_count,
    x_hbm, c_hbm, f_hbm, w_hbm, first_hbm, second_hbm,
    first_ref, second_ref, f_out, normed_out, w_out,
    xbuf, cbuf, wide, first_in, second_in,
    pacc, fbuf, wbuf, pbuf, rbuf, nbuf, sq_own, sq_tp, sq_mid, sq_fs,
    x_sem, c_sem, in_sem, fo_sem, wo_sem,
    f_send, f_recv, d_send, d_recv, w_send, w_recv, p_send, p_recv,
    t_send, t_recv, s_send, s_recv, n_send, n_recv,
):
    me, col = lax.axis_index("fs"), lax.axis_index("tp")
    core = lax.rem(col, 2)
    mate = flip(col, 1, ntp)
    chunks, chunk = xbuf.shape[0], xbuf.shape[1]
    rows = first_in.shape[1]
    half = wbuf.shape[3]
    peers = [flip(me, o, nfs) for o in range(1, nfs)]
    sides = [flip(col, o, ntp) for o in range(1, ntp)]
    odd = lax.rem(me, 2)
    place = (1 - odd) * lax.div(me, 2) + odd * (nfs - 1 - lax.div(me, 2))
    onward = [ring_index(place + 1, nfs), ring_index(place - 1, nfs)]
    hops = [nfs // 2, (nfs - 1) // 2]
    sends = []

    def origin(way, step):
        return ring_index(place - step if way == 0 else place + step, nfs)

    def remote(src, dst, send, recv, fs, tp):
        return pltpu.make_async_remote_copy(
            src_ref=src, dst_ref=dst, send_sem=send, recv_sem=recv,
            device_id=(fs, tp), device_id_type=MESH,
        )

    def begin(copy):
        copy.start()
        sends.append(copy)

    f_copy = pltpu.make_async_copy(f_hbm, fbuf.at[me], in_sem.at[0])
    w_copy = pltpu.make_async_copy(w_hbm, wide, in_sem.at[1])
    moments = [
        pltpu.make_async_copy(first_hbm, first_in, in_sem.at[2]),
        pltpu.make_async_copy(second_hbm, second_in, in_sem.at[3]),
    ]
    x_copies = [
        pltpu.make_async_copy(x_hbm.at[i], xbuf.at[i], x_sem.at[i]) for i in range(chunks)
    ]
    c_copies = [pltpu.make_async_copy(c_hbm.at[m], cbuf.at[m], c_sem.at[m]) for m in range(3)]
    for copy in [f_copy, w_copy] + x_copies + c_copies + moments:
        copy.start()

    barrier = pltpu.get_barrier_semaphore()
    for peer in peers:
        pl.semaphore_signal(barrier, inc=1, device_id=(peer, col), device_id_type=MESH)
    for side in sides:
        pl.semaphore_signal(barrier, inc=1, device_id=(me, side), device_id_type=MESH)
    f_copy.wait()
    w_copy.wait()
    for way in range(2):
        for m in range(3):
            wbuf[me, way, m] = wide[m, way * half:(way + 1) * half, :].astype(jnp.bfloat16)
    pl.semaphore_wait(barrier, nfs - 1 + ntp - 1)

    def pass_weights(way, step, m):
        held = wbuf.at[origin(way, step), way, m]
        return remote(
            held, held, w_send.at[way, m, step], w_recv.at[way, m, origin(way, step)],
            onward[way], col,
        )

    stores = []

    def store_weights(way, step):
        where = origin(way, step)
        copy = pltpu.make_async_copy(
            wbuf.at[where, way], w_out.at[where, way], wo_sem.at[way, step]
        )
        copy.start()
        stores.append(copy)

    ticks = [(step, m) for step in range(1, nfs) for m in range(3)]
    total_ticks = len(ticks)

    def advance(part):
        while ticks and (total_ticks - len(ticks)) * 21 < part * total_ticks:
            step, m = ticks.pop(0)
            for way in range(2):
                pass_weights(way, step, m).wait_recv()
                if step < nfs - 1:
                    begin(pass_weights(way, step, m))
                if m == 2:
                    store_weights(way, step)

    def pass_factor(way, step):
        held = fbuf.at[origin(way, step), core]
        return remote(
            held, held, f_send.at[way, step], f_recv.at[origin(way, step)], onward[way], col
        )

    def share_factor(way, step, which):
        held = fbuf.at[origin(way, step), which]
        return remote(
            held, held, d_send.at[way, step], d_recv.at[origin(way, step)], me, mate
        )

    for way in range(2):
        begin(pass_factor(way, 0))
    for way in range(2):
        for m in range(3):
            begin(pass_weights(way, 0, m))
        store_weights(way, 0)
    for step in range(1, hops[0] + 1):
        for way in range(2):
            if step <= hops[way]:
                pass_factor(way, step).wait_recv()
                if step < hops[way]:
                    begin(pass_factor(way, step))
                begin(share_factor(way, step, core))
        advance((step - 1) * 5 // 3)
    for copy in x_copies + c_copies:
        copy.wait()
    for way in range(2):
        for step in range(1, hops[way] + 1):
            share_factor(way, step, 1 - core).wait_recv()
    fo_copy = pltpu.make_async_copy(fbuf, f_out, fo_sem)
    fo_copy.start()

    pacc[...] = jnp.zeros_like(pacc)
    whole = fbuf.shape[0] * fbuf.shape[1] * fbuf.shape[2]
    for i in range(chunks):
        factor = fbuf[...].reshape(whole, fbuf.shape[3])
        low = jnp.dot(xbuf[i], factor, preferred_element_type=jnp.float32).astype(jnp.bfloat16)
        for m in range(3):
            pacc[m] += lax.dot_general(
                low, cbuf[m, i * chunk:(i + 1) * chunk, :], (((0,), (0,)), ((), ())),
                preferred_element_type=jnp.float32,
            )
        if i < chunks - 1:
            advance(5 + i)

    for m in range(3):
        for j in range(nfs):
            pbuf[j, m] = pacc[m, j * rows:(j + 1) * rows, :].astype(jnp.bfloat16)
    for o, peer in reversed(list(enumerate(peers))):
        begin(remote(pbuf.at[peer], rbuf.at[me], p_send.at[o], p_recv.at[me], peer, col))
    projected = pacc[:, pl.ds(pl.multiple_of(me * rows, rows), rows), :]
    for o, peer in enumerate(peers):
        advance(8 + (o * 3) // len(peers))
        remote(
            pbuf.at[peer], rbuf.at[peer], p_send.at[o], p_recv.at[peer], peer, col
        ).wait_recv()
        projected = projected + rbuf[peer].astype(jnp.float32)

    def spread(value):
        total = jnp.sum(jnp.sum(value, axis=0), axis=0, keepdims=True)
        return jnp.broadcast_to(jnp.sum(total, axis=1, keepdims=True), sq_own.shape)

    own = spread(projected * projected)
    sq_own[...] = own
    sq_tp[col] = own
    for o, side in enumerate(sides):
        begin(remote(sq_own, sq_tp.at[col], t_send.at[o], t_recv.at[col], me, side))
    advance(12)
    for o, side in enumerate(sides):
        remote(sq_own, sq_tp.at[side], t_send.at[o], t_recv.at[side], me, side).wait_recv()
    mid = jnp.sum(sq_tp[...], axis=0)
    sq_mid[...] = mid
    sq_fs[me] = mid
    for o, peer in enumerate(peers):
        begin(remote(sq_mid, sq_fs.at[me], s_send.at[o], s_recv.at[me], peer, col))
    for copy in moments:
        copy.wait()
    advance(14)
    for o, peer in enumerate(peers):
        remote(sq_mid, sq_fs.at[peer], s_send.at[o], s_recv.at[peer], peer, col).wait_recv()
    square_sum = jnp.sum(sq_fs[...], axis=0)[:, :1]

    root_mean = jnp.sqrt(square_sum / scale_count + 1e-06)
    clip_factor = jnp.minimum(1.0, 0.25 / root_mean)
    clipped = clip_factor * projected
    new_first = 0.9 * first_in[...] + 0.1 * clipped
    new_second = 0.95 * second_in[...] + 0.05 * clipped * clipped
    normed = new_first / (jnp.sqrt(new_second) + 1e-08)
    nbuf[me] = normed.astype(jnp.bfloat16)

    def pass_normed(way, step):
        held = nbuf.at[origin(way, step)]
        return remote(
            held, held, n_send.at[way, step], n_recv.at[origin(way, step)], onward[way], col
        )

    for way in range(2):
        begin(pass_normed(way, 0))
    first_ref[...] = new_first
    second_ref[...] = new_second
    for step in range(1, hops[0] + 1):
        advance(14 + (step * 7) // hops[0])
        for way in range(2):
            if step <= hops[way]:
                pass_normed(way, step).wait_recv()
                if step < hops[way]:
                    begin(pass_normed(way, step))
    for m in range(3):
        normed_out[m] = jnp.concatenate(
            [nbuf[j, m].astype(jnp.float32) for j in range(nfs)], axis=0
        ).astype(jnp.bfloat16)
    advance(21)
    fo_copy.wait()
    for copy in stores:
        copy.wait()
    for copy in sends:
        copy.wait_send()


def finish_kernel(
    f_ref, f_all, normed, weights, gathered, first, second,
    update, new_weights, copies, first_out, second_out,
):
    first_out[...] = first[...]
    second_out[...] = second[...]
    step = jnp.dot(f_ref[...], normed[0], preferred_element_type=jnp.float32)
    update[0] = step
    new_weights[0] = weights[0] - 0.02 * step
    pieces, _, _, half, cols = gathered.shape
    for j in range(pieces):
        step = jnp.dot(f_all[j], normed[0], preferred_element_type=jnp.float32)
        copies[0, j * 2 * half:(j + 1) * 2 * half] = (
            gathered[j, :, 0].astype(jnp.float32).reshape(2 * half, cols) - 0.02 * step
        ).astype(jnp.bfloat16)


def on_device(nfs, ntp, inputs, cotangents, factor, weights, first_moment, second_moment):
    tokens, width = inputs.shape
    held, rank = factor.shape
    rows, cols = first_moment.shape[1:]
    chunk = min(512, tokens)
    chunks = tokens // chunk

    dma = pltpu.SemaphoreType.DMA
    vmem = pl.BlockSpec(memory_space=pltpu.VMEM)
    hbm = pl.BlockSpec(memory_space=pl.ANY)
    new_first, new_second, f_all, normed, gathered = pl.pallas_call(
        functools.partial(exchange_kernel, nfs, ntp, 3 * rank * cols * ntp),
        out_shape=(
            jax.ShapeDtypeStruct(first_moment.shape, jnp.float32),
            jax.ShapeDtypeStruct(second_moment.shape, jnp.float32),
            jax.ShapeDtypeStruct((nfs, 2, held // 2, rank), jnp.bfloat16),
            jax.ShapeDtypeStruct((3, rank, cols), jnp.bfloat16),
            jax.ShapeDtypeStruct((nfs, 2, 3, held // 2, cols), jnp.bfloat16),
        ),
        in_specs=[hbm] * 6,
        out_specs=(vmem, vmem, hbm, vmem, hbm),
        scratch_shapes=[
            pltpu.VMEM((chunks, chunk, width), jnp.bfloat16),
            pltpu.VMEM(cotangents.shape, jnp.bfloat16),
            pltpu.VMEM(weights.shape, jnp.float32),
            pltpu.VMEM(first_moment.shape, jnp.float32),
            pltpu.VMEM(second_moment.shape, jnp.float32),
            pltpu.VMEM((3, rank, cols), jnp.float32),
            pltpu.VMEM((nfs, 2, held // 2, rank), jnp.bfloat16),
            pltpu.VMEM((nfs, 2, 3, held // 2, cols), jnp.bfloat16),
            pltpu.VMEM((nfs, 3, rows, cols), jnp.bfloat16),
            pltpu.VMEM((nfs, 3, rows, cols), jnp.bfloat16),
            pltpu.VMEM((nfs, 3, rows, cols), jnp.bfloat16),
            pltpu.VMEM((1, 128), jnp.float32),
            pltpu.VMEM((ntp, 1, 128), jnp.float32),
            pltpu.VMEM((1, 128), jnp.float32),
            pltpu.VMEM((nfs, 1, 128), jnp.float32),
            dma((chunks,)), dma((3,)), dma((4,)), dma, dma((2, nfs)),
            dma((2, nfs)), dma((nfs,)), dma((2, nfs)), dma((nfs,)),
            dma((2, 3, nfs)), dma((2, 3, nfs)), dma((nfs,)), dma((nfs,)),
            dma((ntp,)), dma((ntp,)), dma((nfs,)), dma((nfs,)), dma((2, nfs)), dma((nfs,)),
        ],
        compiler_params=pltpu.CompilerParams(
            collective_id=0, has_side_effects=True, vmem_limit_bytes=63 * 2**20
        ),
        cost_estimate=pl.CostEstimate(
            flops=50_000_000_000, bytes_accessed=100_000_000, transcendentals=0
        ),
        name="exchange",
    )(
        inputs.reshape(chunks, chunk, width), cotangents,
        factor.reshape(2, held // 2, rank), weights, first_moment, second_moment,
    )
    f_all = f_all.reshape(nfs, held, rank)
    update, new_weights, copies, new_first, new_second = pl.pallas_call(
        finish_kernel,
        grid=(3,),
        out_shape=(
            jax.ShapeDtypeStruct(weights.shape, jnp.float32),
            jax.ShapeDtypeStruct(weights.shape, jnp.float32),
            jax.ShapeDtypeStruct((3, nfs * held, cols), jnp.bfloat16),
            jax.ShapeDtypeStruct(first_moment.shape, jnp.float32),
            jax.ShapeDtypeStruct(second_moment.shape, jnp.float32),
        ),
        in_specs=[
            pl.BlockSpec((held, rank), lambda m: (0, 0)),
            pl.BlockSpec((nfs, held, rank), lambda m: (0, 0, 0)),
            pl.BlockSpec((1, rank, cols), lambda m: (m, 0, 0)),
            pl.BlockSpec((1, held, cols), lambda m: (m, 0, 0)),
            pl.BlockSpec((nfs, 2, 1, held // 2, cols), lambda m: (0, 0, m, 0, 0)),
            pl.BlockSpec((1, rows, cols), lambda m: (m, 0, 0)),
            pl.BlockSpec((1, rows, cols), lambda m: (m, 0, 0)),
        ],
        out_specs=(
            pl.BlockSpec((1, held, cols), lambda m: (m, 0, 0)),
            pl.BlockSpec((1, held, cols), lambda m: (m, 0, 0)),
            pl.BlockSpec((1, nfs * held, cols), lambda m: (m, 0, 0)),
            pl.BlockSpec((1, rows, cols), lambda m: (m, 0, 0)),
            pl.BlockSpec((1, rows, cols), lambda m: (m, 0, 0)),
        ),
        name="finish",
    )(factor, f_all, normed, weights, gathered, new_first, new_second)
    return (update, new_weights, copies, new_first, new_second)


def solution(mesh):
    placed = (
        P("fs", None),
        P(None, "fs", "tp"),
        P("fs", None),
        P(None, "fs", "tp"),
        P(None, "fs", "tp"),
        P(None, "fs", "tp"),
    )
    return jax.shard_map(
        functools.partial(on_device, mesh.shape["fs"], mesh.shape["tp"]),
        mesh=mesh,
        in_specs=placed,
        out_specs=(
            P(None, "fs", "tp"),
            P(None, "fs", "tp"),
            P(None, None, "tp"),
            P(None, "fs", "tp"),
            P(None, "fs", "tp"),
        ),
        check_vma=False,
    )
```
